32 devices in a mesh: kv: 16 (over z, y, x), tp: 2 (over core).
Axes of the slice: x: 2, y: 2, z: 4, core: 2. Of those that a mesh axis runs over, the one named last changes fastest.
Arguments:
- tokens: bfloat16 [4096, 2048], P('kv'), may hold values from -40 to 40
- query_weight: bfloat16 [2048, 2048], P(None, 'tp'), may hold values from -0.125 to 0.125
- key_matrix: bfloat16 [2048, 1024], P(None, 'tp'), may hold values from -0.125 to 0.125
- value_matrix: bfloat16 [2048, 1024], P(None, 'tp'), may hold values from -0.125 to 0.125
- gate_weight: bfloat16 [2, 2048, 16], replicated, may hold values from -0.125 to 0.125
- key_pool_weight: float32 [16, 8], replicated, may hold values from -1.5 to 1.5
- value_pool_weight: float32 [16, 8], replicated, may hold values from -1.5 to 1.5
- out_weight: bfloat16 [2048, 2048], P('tp'), may hold values from -0.125 to 0.125
- chosen: int32 [64, 32], P('kv'), may hold values from 0 to 63, as said below
Outputs:
- mixed: bfloat16 [4096, 2048], P(('kv', 'tp'))
- log_sums: float32 [4096, 16], P('kv', 'tp')
The draws below stay inside these ranges and needn't reach their ends.
Inputs may be any that keep to these rules, and one draw needn't show every extreme that they name: `chosen`: row i names only blocks <= i and names block i in its first column; a block may stand several times in a row and counts each time. The rows of one index of kv name, together, at most 2 distinct blocks held by any one other index, and exactly 2 of the index just before it whenever there is one.
All inputs are finite; a program needn't handle non-finite values.
Results may differ from the reference program's by a relative error of at most 0.018.
Values may be sent and summed in bfloat16 or wider, within the bound.
A program may use at most 128 MiB of HBM per device.

```python
import jax
import jax.numpy as jnp
from jax import lax

MODEL_WIDTH = 2048
QUERY_HEADS = 16
KEY_HEADS = 8
HEAD_SIZE = 128
TOKENS_PER_SHARD = 256
BLOCK_LENGTH = 64
POOL_STRIDE = 16
PICKED_BLOCKS = 32
SEQUENCE_LENGTH = 4096
KEY_BLOCK_COUNT = 64
N_TP = 2


def draw_tokens(key, part):
    base = jnp.clip(jax.random.normal(key, (SEQUENCE_LENGTH, MODEL_WIDTH), jnp.float32), -5.0, 5.0)
    return base.astype(jnp.bfloat16)


def draw_chosen(key, part):
    per_dev = TOKENS_PER_SHARD // BLOCK_LENGTH
    devices = SEQUENCE_LENGTH // TOKENS_PER_SHARD
    block_total = devices * per_dev
    keys_list = jax.random.split(jax.random.fold_in(key, 17), 6)
    first_slot = jax.random.randint(keys_list[0], (devices, devices), 0, per_dev)
    second_slot = (first_slot + jax.random.randint(keys_list[1], (devices, devices), 1, per_dev)) % per_dev
    pool_table = jnp.stack([first_slot, second_slot], axis=-1)
    block_ids = jnp.arange(block_total, dtype=jnp.int32)[:, None]
    requester = block_ids // per_dev
    local_pos = block_ids % per_dev
    pick_shape = (block_total, PICKED_BLOCKS)
    draws_a = jax.random.randint(keys_list[2], pick_shape, 0, 1 << 30)
    draws_b = jax.random.randint(keys_list[3], pick_shape, 0, 1 << 30)
    draws_c = jax.random.randint(keys_list[4], pick_shape, 0, 1 << 30)
    draws_d = jax.random.randint(keys_list[5], pick_shape, 0, 1 << 30)
    floor_owner = jnp.maximum(requester, 1)
    owners = jnp.minimum(draws_a % floor_owner, draws_b % floor_owner)
    slot_pick = draws_c % 2
    remote = owners * per_dev + pool_table[requester, owners, slot_pick]
    local_pick = requester * per_dev + draws_d % (local_pos + 1)
    use_local = (requester == 0) | (draws_c // 2 % 4 == 0)
    picked_blocks = jnp.where(use_local, local_pick, remote)
    column = jnp.arange(PICKED_BLOCKS)[None, :]
    leading = (local_pos == 0) & (requester >= 1)
    before = jnp.maximum(requester - 1, 0)
    far_owner = jnp.where(requester >= devices // 2, requester - devices // 2, before)
    picked_blocks = jnp.where(leading & (column == 1), before * per_dev + pool_table[requester, before, 0], picked_blocks)
    picked_blocks = jnp.where(leading & (column == 2), before * per_dev + pool_table[requester, before, 1], picked_blocks)
    picked_blocks = jnp.where(leading & (column == 3), far_owner * per_dev + pool_table[requester, far_owner, 0], picked_blocks)
    picked_blocks = jnp.where(column == 0, block_ids, picked_blocks)
    return picked_blocks.astype(jnp.int32)


def steps_of(stream_key, extent, shards, smallest, high):
    factor_of = 1.0
    for dim, shards_of in shards:
        heights = jax.random.uniform(jax.random.fold_in(jax.random.fold_in(stream_key, 6), dim), (shards_of,), jnp.float32, smallest / len(shards), high / len(shards))
        factor_of = factor_of * jnp.repeat(jnp.exp(heights), extent[dim] // shards_of).reshape((-1,) + (1,) * (len(extent) - 1 - dim))
    return factor_of


def centred(own_key, shape, scale, most, pieces=(), kind=jnp.bfloat16):
    level = steps_of(own_key, shape, pieces, -0.22, 0.18) if pieces else 1.0
    entries = jax.random.normal(own_key, shape, jnp.float32) * scale * level
    return jnp.minimum(jnp.maximum(entries, -most), most).astype(kind)


def setup_inputs(seed: int = 0) -> dict:
    streams_of = jax.random.split(jax.random.key(seed), 10)
    return {
        "tokens": draw_tokens(jax.random.fold_in(streams_of[9], 71), 0),
        "query_weight": centred(streams_of[1], (MODEL_WIDTH, QUERY_HEADS * HEAD_SIZE), MODEL_WIDTH ** -0.5, 0.125, ((1, 2),)),
        "key_matrix": centred(streams_of[2], (MODEL_WIDTH, KEY_HEADS * HEAD_SIZE), MODEL_WIDTH ** -0.5, 0.125, ((1, 2),)),
        "value_matrix": centred(streams_of[3], (MODEL_WIDTH, KEY_HEADS * HEAD_SIZE), MODEL_WIDTH ** -0.5, 0.125, ((1, 2),)),
        "gate_weight": centred(streams_of[4], (2, MODEL_WIDTH, QUERY_HEADS), MODEL_WIDTH ** -0.5, 0.125),
        "key_pool_weight": centred(streams_of[5], (POOL_STRIDE, KEY_HEADS), 0.3, 1.5, (), jnp.float32),
        "value_pool_weight": centred(streams_of[6], (POOL_STRIDE, KEY_HEADS), 0.3, 1.5, (), jnp.float32),
        "out_weight": centred(streams_of[7], (QUERY_HEADS * HEAD_SIZE, MODEL_WIDTH), (QUERY_HEADS * HEAD_SIZE) ** -0.5, 0.125, ((0, 2),)),
        "chosen": draw_chosen(jax.random.fold_in(streams_of[9], 71), 0),
    }


THETA = 10000.0
NEGATIVE = -1e30


def apply_rotary(values_in, positions):
    half_width = values_in.shape[-1] // 2
    inverse = THETA ** (-jnp.arange(half_width, dtype=jnp.float32) / half_width)
    angles = positions.astype(jnp.float32)[:, None] * inverse[None, :]
    cosines = jnp.cos(angles)[:, None, :]
    sines = jnp.sin(angles)[:, None, :]
    front_half = values_in[..., :half_width]
    back_half = values_in[..., half_width:]
    return jnp.concatenate([front_half * cosines - back_half * sines, back_half * cosines + front_half * sines], axis=-1)


def reference(tokens, query_weight, key_matrix, value_matrix, gate_weight, key_pool_weight, value_pool_weight, out_weight, chosen):
    group_count_heads = QUERY_HEADS // KEY_HEADS
    positions = jnp.arange(SEQUENCE_LENGTH, dtype=jnp.int32)
    query_proj = jnp.dot(tokens, query_weight, preferred_element_type=jnp.float32).reshape(SEQUENCE_LENGTH, QUERY_HEADS, HEAD_SIZE)
    key_projected = jnp.dot(tokens, key_matrix, preferred_element_type=jnp.float32).reshape(SEQUENCE_LENGTH, KEY_HEADS, HEAD_SIZE)
    value_projected = jnp.dot(tokens, value_matrix, preferred_element_type=jnp.float32).reshape(SEQUENCE_LENGTH, KEY_HEADS, HEAD_SIZE)
    query_states = apply_rotary(query_proj, positions).astype(jnp.bfloat16)
    key_states = apply_rotary(key_projected, positions).astype(jnp.bfloat16)
    value_states = value_projected.astype(jnp.bfloat16)
    pooled_key_count = SEQUENCE_LENGTH // POOL_STRIDE
    block_ends = POOL_STRIDE * jnp.arange(pooled_key_count, dtype=jnp.int32) + POOL_STRIDE - 1
    compact_keys = apply_rotary(jnp.einsum("cwyi,wy->cyi", key_projected.reshape(pooled_key_count, POOL_STRIDE, KEY_HEADS, HEAD_SIZE), key_pool_weight,
                                    precision=lax.Precision.HIGHEST), block_ends).astype(jnp.bfloat16)
    compact_values = jnp.einsum("cwyi,wy->cyi", value_projected.reshape(pooled_key_count, POOL_STRIDE, KEY_HEADS, HEAD_SIZE), value_pool_weight,
                               precision=lax.Precision.HIGHEST).astype(jnp.bfloat16)
    gate_values = jax.nn.sigmoid(jnp.stack([
        jnp.dot(tokens, gate_weight[0], preferred_element_type=jnp.float32),
        jnp.dot(tokens, gate_weight[1], preferred_element_type=jnp.float32)], axis=0))
    score_scale = HEAD_SIZE ** -0.5
    pooled_keys_f = compact_keys.astype(jnp.float32)
    pooled_values_f = compact_values.astype(jnp.float32)

    def pooled_span(start_point):
        query_row_list = lax.dynamic_slice_in_dim(query_states, start_point, TOKENS_PER_SHARD, 0).reshape(TOKENS_PER_SHARD, KEY_HEADS, group_count_heads, HEAD_SIZE)
        scores = jnp.einsum("qgjd,ngd->gjqn", query_row_list.astype(jnp.float32), pooled_keys_f) * score_scale
        row_pos = start_point + jnp.arange(TOKENS_PER_SHARD, dtype=jnp.int32)
        visible = (block_ends[None, :] <= row_pos[:, None]) | (jnp.arange(pooled_key_count)[None, :] == 0)
        masked = jnp.where(visible, scores, NEGATIVE)
        peak_value = jnp.max(masked, axis=-1, keepdims=True)
        exponent = jnp.where(visible, jnp.exp(masked - peak_value), 0.0)
        weights = (exponent / jnp.sum(exponent, axis=-1, keepdims=True)).astype(jnp.bfloat16)
        span_out = jnp.einsum("gjqn,ngd->qgjd", weights.astype(jnp.float32), pooled_values_f)
        return span_out.reshape(TOKENS_PER_SHARD, QUERY_HEADS, HEAD_SIZE)

    span_starts = TOKENS_PER_SHARD * jnp.arange(SEQUENCE_LENGTH // TOKENS_PER_SHARD, dtype=jnp.int32)
    pooled_out = lax.map(pooled_span, span_starts).reshape(SEQUENCE_LENGTH, QUERY_HEADS, HEAD_SIZE)
    key_block_rows = key_states.reshape(KEY_BLOCK_COUNT, BLOCK_LENGTH, KEY_HEADS, HEAD_SIZE)
    value_block_rows = value_states.reshape(KEY_BLOCK_COUNT, BLOCK_LENGTH, KEY_HEADS, HEAD_SIZE)

    def chosen_block(packed):
        block_number, picked_blocks = packed
        query_row_list = lax.dynamic_slice_in_dim(query_states, block_number * BLOCK_LENGTH, BLOCK_LENGTH, 0).reshape(BLOCK_LENGTH, KEY_HEADS, group_count_heads, HEAD_SIZE)
        key_row_list = key_block_rows[picked_blocks].reshape(PICKED_BLOCKS * BLOCK_LENGTH, KEY_HEADS, HEAD_SIZE).astype(jnp.float32)
        value_row_list = value_block_rows[picked_blocks].reshape(PICKED_BLOCKS * BLOCK_LENGTH, KEY_HEADS, HEAD_SIZE).astype(jnp.float32)
        scores = jnp.einsum("qgjd,kgd->gjqk", query_row_list.astype(jnp.float32), key_row_list) * score_scale
        key_pos = (picked_blocks[:, None] * BLOCK_LENGTH + jnp.arange(BLOCK_LENGTH, dtype=jnp.int32)[None, :]).reshape(-1)
        query_pos = block_number * BLOCK_LENGTH + jnp.arange(BLOCK_LENGTH, dtype=jnp.int32)
        allowed = key_pos[None, :] <= query_pos[:, None]
        masked = jnp.where(allowed, scores, NEGATIVE)
        peak_value = jnp.max(masked, axis=-1, keepdims=True)
        exponent = jnp.where(allowed, jnp.exp(masked - peak_value), 0.0)
        totals = jnp.sum(exponent, axis=-1, keepdims=True)
        weights = (exponent / totals).astype(jnp.bfloat16)
        block_out = jnp.einsum("gjqk,kgd->qgjd", weights.astype(jnp.float32), value_row_list).reshape(BLOCK_LENGTH, QUERY_HEADS, HEAD_SIZE)
        block_logs = jnp.transpose((peak_value + jnp.log(totals))[..., 0], (2, 0, 1)).reshape(BLOCK_LENGTH, QUERY_HEADS)
        return block_out, block_logs

    sel_out, log_sums = lax.map(chosen_block, (jnp.arange(KEY_BLOCK_COUNT, dtype=jnp.int32), chosen))
    sel_out = sel_out.reshape(SEQUENCE_LENGTH, QUERY_HEADS, HEAD_SIZE)
    log_sums = log_sums.reshape(SEQUENCE_LENGTH, QUERY_HEADS)
    attended = (gate_values[0][:, :, None] * pooled_out + gate_values[1][:, :, None] * sel_out)
    attended = attended.astype(jnp.bfloat16).reshape(SEQUENCE_LENGTH, QUERY_HEADS * HEAD_SIZE)
    group_width = QUERY_HEADS * HEAD_SIZE // N_TP
    summed = jnp.zeros((SEQUENCE_LENGTH, MODEL_WIDTH), jnp.float32)
    for member in range(N_TP):
        partial_value = jnp.dot(attended[:, member * group_width:(member + 1) * group_width],
                          out_weight[member * group_width:(member + 1) * group_width],
                          preferred_element_type=jnp.float32).astype(jnp.bfloat16)
        partial_value = lax.optimization_barrier(partial_value)
        summed = summed + partial_value.astype(jnp.float32)
    return summed.astype(jnp.bfloat16), log_sums
```

```python
import functools
import math

import jax
import jax.numpy as jnp
from jax import lax
from jax.experimental import pallas as pl
from jax.experimental.pallas import tpu as pltpu
from jax.sharding import PartitionSpec as P

HEAD_SIZE = 128
BLOCK_LENGTH = 64
POOL_STRIDE = 16
THETA = 10000.0
NEGATIVE = -1e30
SCALE2 = math.log2(math.e) / math.sqrt(HEAD_SIZE)
LN2 = math.log(2.0)
MESH = pl.DeviceIdType.MESH


def nt(a, b):
    return lax.dot_general(a, b, (((1,), (1,)), ((), ())), preferred_element_type=jnp.float32)


def rotate(x, cosines, sines):
    return x * cosines + pltpu.roll(x, HEAD_SIZE // 2, 1) * sines


def project_kernel(
    r, tokens, wq, wk, wv, gw, cos, sin, cosp, sinp, mixk, mixv, q_out, k_out, v_out, g_out
):
    rows = tokens.shape[0]
    pooled = rows // POOL_STRIDE
    x = tokens[...]
    q = jnp.dot(x, wq[...], preferred_element_type=jnp.float32)
    for j in range(r):
        part = q[:, j * HEAD_SIZE : (j + 1) * HEAD_SIZE]
        q_out[0, :, j * HEAD_SIZE : (j + 1) * HEAD_SIZE] = rotate(part, cos[...], sin[...]).astype(
            jnp.bfloat16
        )
    k = jnp.dot(x, wk[...], preferred_element_type=jnp.float32)
    v = jnp.dot(x, wv[...], preferred_element_type=jnp.float32)
    k_out[0, 0:rows, :] = rotate(k, cos[...], sin[...]).astype(jnp.bfloat16)
    kp = jnp.dot(
        mixk[0], k, preferred_element_type=jnp.float32, precision=lax.Precision.HIGHEST
    )
    vp = jnp.dot(
        mixv[0], v, preferred_element_type=jnp.float32, precision=lax.Precision.HIGHEST
    )
    k_out[0, rows : rows + pooled, :] = rotate(kp, cosp[...], sinp[...]).astype(jnp.bfloat16)
    k_out[0, rows + pooled : rows + 2 * pooled, :] = vp.astype(jnp.bfloat16)
    v_out[0] = v.T.astype(jnp.bfloat16)

    @pl.when(pl.program_id(0) == 0)
    def _():
        heads = gw.shape[2]
        for b in range(2):
            logits = lax.dot_general(
                gw[b], x, (((0,), (1,)), ((), ())), preferred_element_type=jnp.float32
            )
            g_out[b * heads : (b + 1) * heads, :] = jax.nn.sigmoid(logits)


def attend_kernel(
    dims,
    q_in,
    k_in,
    v_in,
    cnt_in,
    g_in,
    wo_in,
    mixed,
    lse_out,
    qbuf,
    kbuf,
    vbuf,
    cbuf,
    gbuf,
    wo,
    bias_ref,
    acc,
    mref,
    lref,
    pacc,
    pmref,
    plref,
    obox,
    lbox,
    abuf,
    lbuf,
    sbox,
    rbox,
    local_sem,
    send_sem,
    recv_sem,
    chain_send,
    chain_recv,
    back_send,
    back_recv,
    tp_send,
    tp_recv,
):
    G, Z, T, R, r, H = dims
    nb = G * (R // BLOCK_LENGTH)
    pooled = R // POOL_STRIDE
    kv = lax.axis_index("kv")
    t = lax.axis_index("tp")
    c = lax.rem(kv, G)
    z = kv // G

    def member(g):
        return lax.rem(c + g, G)

    def at(group, who):
        return {"kv": group * G + who}

    barrier = pltpu.get_barrier_semaphore()
    for g in range(1, G):
        pl.semaphore_signal(barrier, inc=1, device_id=at(z, member(g)), device_id_type=MESH)
    for d in (1, Z - 1):
        pl.semaphore_signal(
            barrier, inc=1, device_id=at(lax.rem(z + d, Z), c), device_id_type=MESH
        )
    for o in range(1, T):
        pl.semaphore_signal(
            barrier, inc=1, device_id={"tp": lax.rem(t + o, T)}, device_id_type=MESH
        )
    wo_copy = pltpu.make_async_copy(wo_in, wo, local_sem.at[5])
    wo_copy.start()
    locals_ = [
        pltpu.make_async_copy(k_in.at[c], kbuf.at[0, c], local_sem.at[0]),
        pltpu.make_async_copy(v_in.at[c], vbuf.at[0, c], local_sem.at[1]),
        pltpu.make_async_copy(q_in.at[c], qbuf.at[c], local_sem.at[2]),
        pltpu.make_async_copy(cnt_in, cbuf.at[c], local_sem.at[3]),
        pltpu.make_async_copy(g_in, gbuf.at[c], local_sem.at[4]),
    ]
    for copy in locals_:
        copy.start()
    pl.semaphore_wait(barrier, G - 1 + 2 + T - 1)

    swaps = []
    for i in range(5):
        for g in range(1, G):
            who = member(g)
            src, dst = [
                (k_in.at[who], kbuf.at[0, c]),
                (v_in.at[who], vbuf.at[0, c]),
                (q_in.at[who], qbuf.at[c]),
                (cnt_in, cbuf.at[c]),
                (g_in, gbuf.at[c]),
            ][i]
            copy = pltpu.make_async_remote_copy(
                src_ref=src,
                dst_ref=dst,
                send_sem=send_sem.at[i, g],
                recv_sem=recv_sem.at[i, g],
                device_id=at(z, who),
                device_id_type=MESH,
            )
            copy.start()
            swaps.append(copy)

    def chain(s):
        up = at(lax.rem(z + 1, Z), c)
        return [
            pltpu.make_async_remote_copy(
                src_ref=buf.at[s],
                dst_ref=buf.at[s + 1],
                send_sem=chain_send.at[i, s],
                recv_sem=chain_recv.at[i, s],
                device_id=up,
                device_id_type=MESH,
            )
            for i, buf in ((0, kbuf), (1, vbuf))
        ]

    for copy in locals_[:2]:
        copy.wait()
    for copy in swaps[: 2 * (G - 1)]:
        copy.wait_recv()

    @pl.when(z + 1 < Z)
    def _():
        for copy in chain(0):
            copy.start()

    for copy in locals_[2:]:
        copy.wait()
    for copy in swaps[2 * (G - 1) :]:
        copy.wait_recv()

    lanes_q = lax.broadcasted_iota(jnp.int32, (128, R), 1) // BLOCK_LENGTH
    spread = (lanes_q == lax.broadcasted_iota(jnp.int32, (128, R), 0)).astype(jnp.bfloat16)

    def make_bias(n, carry):
        who, plane = n // Z, lax.rem(n, Z)
        counts = jnp.dot(
            cbuf[who, plane].astype(jnp.bfloat16), spread, preferred_element_type=jnp.float32
        )
        bias_ref[who, plane] = jnp.where(
            counts > 0.5, jnp.log2(jnp.maximum(counts, 1.0)), NEGATIVE
        )
        return carry

    lax.fori_loop(0, G * Z, make_bias, 0)

    def attend(s, first):
        plane = z - s

        def chunk(n, carry):
            cq, j = n // r, lax.rem(n, r)
            q = qbuf[cq, :, pl.ds(pl.multiple_of(j * HEAD_SIZE, HEAD_SIZE), HEAD_SIZE)]
            bias = bias_ref[cq, plane]
            st = jnp.concatenate([nt(kbuf[s, a, 0:R, :], q) for a in range(G)], axis=0) * SCALE2
            st = st.reshape(nb, BLOCK_LENGTH, R) + bias[:nb].reshape(nb, 1, R)
            st = st.reshape(G * R, R)
            if first:
                keys = lax.broadcasted_iota(jnp.int32, (G * R, R), 0)
                queries = lax.broadcasted_iota(jnp.int32, (G * R, R), 1) + cq * R
                st = jnp.where(keys <= queries, st, NEGATIVE)
            kp = kbuf[s, :, R : R + pooled, :].reshape(G * pooled, HEAD_SIZE)
            vp = kbuf[s, :, R + pooled : R + 2 * pooled, :].reshape(G * pooled, HEAD_SIZE)
            index = plane * (G * pooled) + lax.broadcasted_iota(jnp.int32, (G * pooled, R), 0)
            where_q = (z * G + cq) * R + lax.broadcasted_iota(jnp.int32, (G * pooled, R), 1)
            seen = (POOL_STRIDE * index + POOL_STRIDE - 1 <= where_q) | (index == 0)
            sp = jnp.where(seen, nt(kp, q) * SCALE2, NEGATIVE)
            peak = jnp.max(st, axis=0, keepdims=True)
            ppeak = jnp.max(sp, axis=0, keepdims=True)
            if not first:
                peak = jnp.maximum(peak, mref[cq, j])
                ppeak = jnp.maximum(ppeak, pmref[cq, j])
            e = jnp.exp2(st - peak)
            pe = jnp.exp2(sp - ppeak)
            total = jnp.sum(e, axis=0, keepdims=True)
            ptotal = jnp.sum(pe, axis=0, keepdims=True)
            eb = e.astype(jnp.bfloat16)
            out = jnp.dot(vbuf[s, 0], eb[0:R], preferred_element_type=jnp.float32)
            for a in range(1, G):
                out += jnp.dot(
                    vbuf[s, a], eb[a * R : (a + 1) * R], preferred_element_type=jnp.float32
                )
            pout = lax.dot_general(
                vp,
                pe.astype(jnp.bfloat16),
                (((0,), (0,)), ((), ())),
                preferred_element_type=jnp.float32,
            )
            if not first:
                shrink = jnp.exp2(mref[cq, j] - peak)
                pshrink = jnp.exp2(pmref[cq, j] - ppeak)
                total += lref[cq, j] * shrink
                ptotal += plref[cq, j] * pshrink
                out += acc[cq, j] * shrink
                pout += pacc[cq, j] * pshrink
            mref[cq, j] = peak
            lref[cq, j] = total
            acc[cq, j] = out
            pmref[cq, j] = ppeak
            plref[cq, j] = ptotal
            pacc[cq, j] = pout
            return carry

        lax.fori_loop(0, G * r, chunk, 0)

    attend(0, True)

    def step(s, carry):
        for copy in chain(s - 1):
            copy.wait_recv()

        @pl.when(z + 1 < Z)
        def _():
            for copy in chain(s):
                copy.start()

        attend(s, False)
        return carry

    lax.fori_loop(1, z + 1, step, 0)

    backs = []
    for g in list(range(1, G)) + [0]:
        who = member(g)
        for j in range(r):
            head = t * (G * r) + c * r + j
            gate_p = gbuf[who, pl.ds(head, 1), :]
            gate_s = gbuf[who, pl.ds(H + head, 1), :]
            total = lref[who, j]
            mixed_t = pacc[who, j] * (gate_p / plref[who, j]) + acc[who, j] * (gate_s / total)
            obox[g, :, j * HEAD_SIZE : (j + 1) * HEAD_SIZE] = mixed_t.T.astype(jnp.bfloat16)
            lbox[g, j : j + 1, :] = (mref[who, j] + jnp.log2(total)) * LN2
        if g:
            for i, (src, dst) in enumerate(((obox.at[g], abuf.at[c]), (lbox.at[g], lbuf.at[c]))):
                copy = pltpu.make_async_remote_copy(
                    src_ref=src,
                    dst_ref=dst,
                    send_sem=back_send.at[i, g],
                    recv_sem=back_recv.at[i, g],
                    device_id=at(z, who),
                    device_id_type=MESH,
                )
                copy.start()
                backs.append(copy)
    abuf[c] = obox[0]
    lbuf[c] = lbox[0]
    wo_copy.wait()
    for copy in backs:
        copy.wait_recv()
    lse_out[...] = lbuf[...]

    width = wo.shape[1]
    piece = R // T
    span = r * HEAD_SIZE

    def share(dest):
        rows = pl.ds(pl.multiple_of(dest * piece, piece), piece)
        total = None
        for a in range(G):
            term = jnp.dot(
                abuf[a, rows, :],
                wo[a * span : (a + 1) * span, :],
                preferred_element_type=jnp.float32,
            )
            total = term if total is None else total + term
        return total.astype(jnp.bfloat16)

    hops = []
    for o in range(1, T):
        dest = lax.rem(t + o, T)
        sbox[o] = share(dest)
        copy = pltpu.make_async_remote_copy(
            src_ref=sbox.at[o],
            dst_ref=rbox.at[o],
            send_sem=tp_send.at[o],
            recv_sem=tp_recv.at[o],
            device_id={"tp": dest},
            device_id_type=MESH,
        )
        copy.start()
        hops.append(copy)
    final = share(t).astype(jnp.float32)
    for o in range(1, T):
        hops[o - 1].wait_recv()
        final = final + rbox[o].astype(jnp.float32)
    mixed[...] = final.astype(jnp.bfloat16)

    for copy in swaps + backs + hops:
        copy.wait_send()

    @pl.when(z + 1 < Z)
    def _():
        def drain(s, carry):
            for copy in chain(s):
                copy.wait_send()
            return carry

        lax.fori_loop(0, z + 1, drain, 0)


def shards(
    tokens,
    query_weight,
    key_matrix,
    value_matrix,
    gate_weight,
    key_pool_weight,
    value_pool_weight,
    out_weight,
    chosen,
):
    R, width = tokens.shape
    kv_size = lax.axis_size("kv")
    T = lax.axis_size("tp")
    kv = lax.axis_index("kv")
    t = lax.axis_index("tp")
    G = key_matrix.shape[1] // HEAD_SIZE
    r = query_weight.shape[1] // key_matrix.shape[1]
    Z = kv_size // G
    H = gate_weight.shape[2]
    per_dev = chosen.shape[0]
    pooled = R // POOL_STRIDE
    nb = G * per_dev
    nbp = max(8, nb)
    span = r * HEAD_SIZE
    f32, bf16 = jnp.float32, jnp.bfloat16

    half = HEAD_SIZE // 2
    lane = jnp.arange(HEAD_SIZE, dtype=jnp.int32)
    inverse = THETA ** (-(lane % half).astype(f32) / half)
    positions = kv * R + jnp.arange(R, dtype=jnp.int32)
    angles = positions.astype(f32)[:, None] * inverse[None, :]
    cos = jnp.cos(angles)
    sin = jnp.sin(angles) * jnp.where(lane < half, -1.0, 1.0)[None, :]
    cosp = cos[POOL_STRIDE - 1 :: POOL_STRIDE]
    sinp = sin[POOL_STRIDE - 1 :: POOL_STRIDE]

    own = jnp.arange(R)[None, :] // POOL_STRIDE == jnp.arange(pooled)[:, None]

    def mixer(weights):
        mine = lax.dynamic_slice_in_dim(weights, t * G, G, 1).T
        return jnp.where(own[None], jnp.tile(mine, (1, pooled))[:, None, :], 0.0)

    once = lambda *shape: pl.BlockSpec(shape, lambda g: (0,) * len(shape))
    q_all, k_all, v_all, gates = pl.pallas_call(
        functools.partial(project_kernel, r),
        grid=(G,),
        in_specs=[
            once(R, width),
            pl.BlockSpec((width, span), lambda g: (0, g)),
            pl.BlockSpec((width, HEAD_SIZE), lambda g: (0, g)),
            pl.BlockSpec((width, HEAD_SIZE), lambda g: (0, g)),
            once(2, width, H),
            once(R, HEAD_SIZE),
            once(R, HEAD_SIZE),
            once(pooled, HEAD_SIZE),
            once(pooled, HEAD_SIZE),
            pl.BlockSpec((1, pooled, R), lambda g: (g, 0, 0)),
            pl.BlockSpec((1, pooled, R), lambda g: (g, 0, 0)),
        ],
        out_specs=[
            pl.BlockSpec((1, R, span), lambda g: (g, 0, 0)),
            pl.BlockSpec((1, R + 2 * pooled, HEAD_SIZE), lambda g: (g, 0, 0)),
            pl.BlockSpec((1, HEAD_SIZE, R), lambda g: (g, 0, 0)),
            once(2 * H, R),
        ],
        out_shape=[
            jax.ShapeDtypeStruct((G, R, span), bf16),
            jax.ShapeDtypeStruct((G, R + 2 * pooled, HEAD_SIZE), bf16),
            jax.ShapeDtypeStruct((G, HEAD_SIZE, R), bf16),
            jax.ShapeDtypeStruct((2 * H, R), f32),
        ],
        name="project",
    )(
        tokens,
        query_weight,
        key_matrix,
        value_matrix,
        gate_weight,
        cos,
        sin,
        cosp,
        sinp,
        mixer(key_pool_weight),
        mixer(value_pool_weight),
    )

    blocks = jnp.arange(kv_size * per_dev, dtype=jnp.int32)
    counts = jnp.sum((chosen[None] == blocks[:, None, None]).astype(f32), axis=2)
    counts = jnp.pad(counts.reshape(Z, nb, per_dev), ((0, 0), (0, nbp - nb), (0, 128 - per_dev)))

    vmem = pl.BlockSpec(memory_space=pltpu.VMEM)
    anywhere = pl.BlockSpec(memory_space=pl.ANY)
    sem = pltpu.SemaphoreType.DMA
    mixed, lse = pl.pallas_call(
        functools.partial(attend_kernel, (G, Z, T, R, r, H)),
        in_specs=[anywhere] * 6,
        out_specs=[vmem, vmem],
        out_shape=[
            jax.ShapeDtypeStruct((R // T, out_weight.shape[1]), bf16),
            jax.ShapeDtypeStruct((G, 8, R), f32),
        ],
        scratch_shapes=[
            pltpu.VMEM((G, R, span), bf16),
            pltpu.VMEM((Z, G, R + 2 * pooled, HEAD_SIZE), bf16),
            pltpu.VMEM((Z, G, HEAD_SIZE, R), bf16),
            pltpu.VMEM((G, Z, nbp, 128), f32),
            pltpu.VMEM((G, 2 * H, R), f32),
            pltpu.VMEM(out_weight.shape, bf16),
            pltpu.VMEM((G, Z, nbp, R), f32),
            pltpu.VMEM((G, r, HEAD_SIZE, R), f32),
            pltpu.VMEM((G, r, 1, R), f32),
            pltpu.VMEM((G, r, 1, R), f32),
            pltpu.VMEM((G, r, HEAD_SIZE, R), f32),
            pltpu.VMEM((G, r, 1, R), f32),
            pltpu.VMEM((G, r, 1, R), f32),
            pltpu.VMEM((G, R, span), bf16),
            pltpu.VMEM((G, 8, R), f32),
            pltpu.VMEM((G, R, span), bf16),
            pltpu.VMEM((G, 8, R), f32),
            pltpu.VMEM((T, R // T, out_weight.shape[1]), bf16),
            pltpu.VMEM((T, R // T, out_weight.shape[1]), bf16),
            sem((6,)),
            sem((5, G)),
            sem((5, G)),
            sem((2, Z)),
            sem((2, Z)),
            sem((2, G)),
            sem((2, G)),
            sem((T,)),
            sem((T,)),
        ],
        compiler_params=pltpu.CompilerParams(collective_id=0, has_side_effects=True),
        name="attend",
    )(q_all, k_all, v_all, counts, gates, out_weight)
    log_sums = lse[:, :r, :].reshape(G * r, R).T
    return mixed, log_sums


def solution(mesh):
    in_specs = (
        P("kv", None),
        P(None, "tp"),
        P(None, "tp"),
        P(None, "tp"),
        P(),
        P(),
        P(),
        P("tp", None),
        P("kv", None),
    )
    out_specs = (P(("kv", "tp"), None), P("kv", "tp"))
    return jax.shard_map(shards, mesh=mesh, in_specs=in_specs, out_specs=out_specs, check_vma=False)
```

```python
import functools
import math

import jax
import jax.numpy as jnp
from jax import lax
from jax.experimental import pallas as pl
from jax.experimental.pallas import tpu as pltpu
from jax.sharding import PartitionSpec as P

HEAD_SIZE = 128
BLOCK_LENGTH = 64
POOL_STRIDE = 16
THETA = 10000.0
NEGATIVE = -1e30
SCALE2 = math.log2(math.e) / math.sqrt(HEAD_SIZE)
LN2 = math.log(2.0)
MESH = pl.DeviceIdType.MESH


def nt(a, b):
    return lax.dot_general(a, b, (((1,), (1,)), ((), ())), preferred_element_type=jnp.float32)


def rotate(x, cosines, sines):
    return x * cosines + pltpu.roll(x, HEAD_SIZE // 2, 1) * sines


def pool_matrix(weights, head, rows):
    pooled = rows // POOL_STRIDE
    row = weights[pl.ds(head, 1), :]
    shape = (POOL_STRIDE, POOL_STRIDE)
    eye = lax.broadcasted_iota(jnp.int32, shape, 0) == lax.broadcasted_iota(jnp.int32, shape, 1)
    column = jnp.sum(jnp.where(eye, row, 0.0), axis=1, keepdims=True)
    wide = (POOL_STRIDE, rows)
    match = lax.broadcasted_iota(jnp.int32, wide, 0) == lax.rem(
        lax.broadcasted_iota(jnp.int32, wide, 1), POOL_STRIDE
    )
    tiled = jnp.sum(jnp.where(match, column, 0.0), axis=0, keepdims=True)
    tall = (pooled, rows)
    own = lax.broadcasted_iota(jnp.int32, tall, 0) == (
        lax.broadcasted_iota(jnp.int32, tall, 1) // POOL_STRIDE
    )
    return jnp.where(own, tiled, 0.0)


def attend_kernel(
    dims,
    x_in,
    wq_in,
    wk_in,
    wv_in,
    wo_in,
    cnt_in,
    gw,
    kpool,
    vpool,
    cos,
    sin,
    mixed,
    lse_out,
    x,
    wq,
    wkv,
    wo,
    qst,
    kst,
    vst,
    gst,
    qbuf,
    kbuf,
    vbuf,
    cbuf,
    gbuf,
    bias_ref,
    acc,
    mref,
    lref,
    pacc,
    pmref,
    plref,
    obox,
    lbox,
    abuf,
    lbuf,
    sbox,
    rbox,
    local_sem,
    weight_sem,
    send_sem,
    recv_sem,
    chain_send,
    chain_recv,
    back_send,
    back_recv,
    tp_send,
    tp_recv,
):
    G, Z, T, R, r, H = dims
    nb = G * (R // BLOCK_LENGTH)
    pooled = R // POOL_STRIDE
    span = r * HEAD_SIZE
    kv = lax.axis_index("kv")
    t = lax.axis_index("tp")
    c = lax.rem(kv, G)
    z = kv // G

    def member(g):
        return lax.rem(c + g, G)

    def at(group, who):
        return {"kv": group * G + who}

    barrier = pltpu.get_barrier_semaphore()
    for g in range(1, G):
        pl.semaphore_signal(barrier, inc=1, device_id=at(z, member(g)), device_id_type=MESH)
    for d in (1, Z - 1):
        pl.semaphore_signal(
            barrier, inc=1, device_id=at(lax.rem(z + d, Z), c), device_id_type=MESH
        )
    for o in range(1, T):
        pl.semaphore_signal(
            barrier, inc=1, device_id={"tp": lax.rem(t + o, T)}, device_id_type=MESH
        )

    x_copy = pltpu.make_async_copy(x_in, x, local_sem.at[0])
    x_copy.start()
    key_copies, query_copies = [], []
    for g in range(G):
        cols = pl.ds(pl.multiple_of(member(g) * HEAD_SIZE, HEAD_SIZE), HEAD_SIZE)
        pair = (
            pltpu.make_async_copy(
                wk_in.at[:, cols], wkv.at[g, :, pl.ds(0, HEAD_SIZE)], weight_sem.at[0, g]
            ),
            pltpu.make_async_copy(
                wv_in.at[:, cols], wkv.at[g, :, pl.ds(HEAD_SIZE, HEAD_SIZE)], weight_sem.at[1, g]
            ),
        )
        for copy in pair:
            copy.start()
        key_copies.append(pair)
    for g in list(range(1, G)) + [0]:
        cols = pl.ds(pl.multiple_of(member(g) * span, span), span)
        copy = pltpu.make_async_copy(wq_in.at[:, cols], wq.at[g], weight_sem.at[2, g])
        copy.start()
        query_copies.append(copy)
    cnt_copy = pltpu.make_async_copy(cnt_in, cbuf.at[c], local_sem.at[1])
    cnt_copy.start()
    wo_copy = pltpu.make_async_copy(wo_in, wo, local_sem.at[2])
    wo_copy.start()

    def swap(i, g):
        src, dst = [
            (kst.at[g], kbuf.at[0, c]),
            (vst.at[g], vbuf.at[0, c]),
            (qst.at[g], qbuf.at[c]),
            (cnt_in, cbuf.at[c]),
            (gst, gbuf.at[c]),
        ][i]
        return pltpu.make_async_remote_copy(
            src_ref=src,
            dst_ref=dst,
            send_sem=send_sem.at[i, g],
            recv_sem=recv_sem.at[i, g],
            device_id=at(z, member(g)),
            device_id_type=MESH,
        )

    def chain(s, g):
        up = at(lax.rem(z + 1, Z), c)
        source = lax.rem(c + G - g, G)
        return [
            pltpu.make_async_remote_copy(
                src_ref=buf.at[s, source],
                dst_ref=buf.at[s + 1, source],
                send_sem=chain_send.at[i, s, g],
                recv_sem=chain_recv.at[i, s, g],
                device_id=up,
                device_id_type=MESH,
            )
            for i, buf in ((0, kbuf), (1, vbuf))
        ]

    def forward(s, g):
        @pl.when(z + 1 < Z)
        def _():
            for copy in chain(s, g):
                copy.start()

    def pass_on(s, g):
        @pl.when(s <= z)
        def _():
            for copy in chain(s - 1, g):
                copy.wait_recv()
            forward(s, g)

    pl.semaphore_wait(barrier, G - 1 + 2 + T - 1)
    x_copy.wait()
    for g in range(G):
        for copy in key_copies[g]:
            copy.wait()
        head = t * G + member(g)
        both = jnp.dot(x[...], wkv[g], preferred_element_type=jnp.float32)
        k, v = both[:, :HEAD_SIZE], both[:, HEAD_SIZE:]
        kp = jnp.dot(
            pool_matrix(kpool, head, R),
            k,
            preferred_element_type=jnp.float32,
            precision=lax.Precision.HIGHEST,
        )
        vp = jnp.dot(
            pool_matrix(vpool, head, R),
            v,
            preferred_element_type=jnp.float32,
            precision=lax.Precision.HIGHEST,
        )
        ends = pl.ds(POOL_STRIDE - 1, pooled, stride=POOL_STRIDE)
        rows_k = rotate(k, cos[...], sin[...]).astype(jnp.bfloat16)
        rows_p = rotate(kp, cos[ends, :], sin[ends, :]).astype(jnp.bfloat16)
        k_to, v_to = (kbuf.at[0, c], vbuf.at[0, c]) if g == 0 else (kst.at[g], vst.at[g])
        k_to[0:R, :] = rows_k
        k_to[R : R + pooled, :] = rows_p
        k_to[R + pooled : R + 2 * pooled, :] = vp.astype(jnp.bfloat16)
        v_to[...] = v.T.astype(jnp.bfloat16)
        if g == 0:
            forward(0, 0)
        else:
            swap(0, g).start()
            swap(1, g).start()
    for n, g in enumerate(list(range(1, G)) + [0]):
        query_copies[n].wait()
        q = jnp.dot(x[...], wq[g], preferred_element_type=jnp.float32)
        q_to = qst.at[g] if g else qbuf.at[c]
        for j in range(r):
            cols = slice(j * HEAD_SIZE, (j + 1) * HEAD_SIZE)
            q_to[:, cols] = rotate(q[:, cols], cos[...], sin[...]).astype(jnp.bfloat16)
        if g:
            swap(2, g).start()
            swap(0, g).wait_recv()
            swap(1, g).wait_recv()
            forward(0, g)
    for b in range(2):
        gst[b * H : (b + 1) * H, :] = jax.nn.sigmoid(nt(gw[b], x[...]))
    gbuf[c] = gst[...]
    for i in (3, 4):
        for g in range(1, G):
            swap(i, g).start()
    cnt_copy.wait()
    early = G // 2
    for g in range(early):
        pass_on(1, g)
    for i in (2, 3, 4):
        for g in range(1, G):
            swap(i, g).wait_recv()

    lanes_q = lax.broadcasted_iota(jnp.int32, (128, R), 1) // BLOCK_LENGTH
    spread = (lanes_q == lax.broadcasted_iota(jnp.int32, (128, R), 0)).astype(jnp.bfloat16)

    def make_bias(n, carry):
        who, plane = n // Z, lax.rem(n, Z)
        counts = jnp.dot(
            cbuf[who, plane].astype(jnp.bfloat16), spread, preferred_element_type=jnp.float32
        )
        bias_ref[who, plane] = jnp.where(
            counts > 0.5, jnp.log2(jnp.maximum(counts, 1.0)), NEGATIVE
        )
        return carry

    lax.fori_loop(0, G * Z, make_bias, 0)

    def chunk(s, first, cq, j):
        plane = z - s
        q = qbuf[cq, :, j * HEAD_SIZE : (j + 1) * HEAD_SIZE]
        bias = bias_ref[cq, plane]
        st = jnp.concatenate([nt(kbuf[s, a, 0:R, :], q) for a in range(G)], axis=0) * SCALE2
        st = st.reshape(nb, BLOCK_LENGTH, R) + bias[:nb].reshape(nb, 1, R)
        st = st.reshape(G * R, R)
        if first:
            keys = lax.broadcasted_iota(jnp.int32, (G * R, R), 0)
            queries = lax.broadcasted_iota(jnp.int32, (G * R, R), 1) + cq * R
            st = jnp.where(keys <= queries, st, NEGATIVE)
        kp = kbuf[s, :, R : R + pooled, :].reshape(G * pooled, HEAD_SIZE)
        vp = kbuf[s, :, R + pooled : R + 2 * pooled, :].reshape(G * pooled, HEAD_SIZE)
        index = plane * (G * pooled) + lax.broadcasted_iota(jnp.int32, (G * pooled, R), 0)
        where_q = (z * G + cq) * R + lax.broadcasted_iota(jnp.int32, (G * pooled, R), 1)
        seen = (POOL_STRIDE * index + POOL_STRIDE - 1 <= where_q) | (index == 0)
        sp = jnp.where(seen, nt(kp, q) * SCALE2, NEGATIVE)
        peak = jnp.max(st, axis=0, keepdims=True)
        ppeak = jnp.max(sp, axis=0, keepdims=True)
        if not first:
            peak = jnp.maximum(peak, mref[cq, j])
            ppeak = jnp.maximum(ppeak, pmref[cq, j])
        e = jnp.exp2(st - peak)
        pe = jnp.exp2(sp - ppeak)
        total = jnp.sum(e, axis=0, keepdims=True)
        ptotal = jnp.sum(pe, axis=0, keepdims=True)
        eb = e.astype(jnp.bfloat16)
        out = jnp.dot(vbuf[s, 0], eb[0:R], preferred_element_type=jnp.float32)
        for a in range(1, G):
            out += jnp.dot(
                vbuf[s, a], eb[a * R : (a + 1) * R], preferred_element_type=jnp.float32
            )
        pout = lax.dot_general(
            vp,
            pe.astype(jnp.bfloat16),
            (((0,), (0,)), ((), ())),
            preferred_element_type=jnp.float32,
        )
        if not first:
            shrink = jnp.exp2(mref[cq, j] - peak)
            pshrink = jnp.exp2(pmref[cq, j] - ppeak)
            total += lref[cq, j] * shrink
            ptotal += plref[cq, j] * pshrink
            out += acc[cq, j] * shrink
            pout += pacc[cq, j] * pshrink
        mref[cq, j] = peak
        lref[cq, j] = total
        acc[cq, j] = out
        pmref[cq, j] = ppeak
        plref[cq, j] = ptotal
        pacc[cq, j] = pout

    def back(i, n):
        src, dst = ((obox.at[n], abuf.at[c]), (lbox.at[n], lbuf.at[c]))[i]
        return pltpu.make_async_remote_copy(
            src_ref=src,
            dst_ref=dst,
            send_sem=back_send.at[i, n],
            recv_sem=back_recv.at[i, n],
            device_id=at(z, member(n + 1)),
            device_id_type=MESH,
        )

    def finish(n, who):
        for j in range(r):
            head = t * (G * r) + c * r + j
            gate_p = gbuf[who, pl.ds(head, 1), :]
            gate_s = gbuf[who, pl.ds(H + head, 1), :]
            total = lref[who, j]
            mixed_t = pacc[who, j] * (gate_p / plref[who, j]) + acc[who, j] * (gate_s / total)
            obox[n, :, j * HEAD_SIZE : (j + 1) * HEAD_SIZE] = mixed_t.T.astype(jnp.bfloat16)
            lbox[n, j : j + 1, :] = (mref[who, j] + jnp.log2(total)) * LN2

        @pl.when(n < G - 1)
        def _():
            back(0, n).start()
            back(1, n).start()

    def attend(s, first):
        def body(n, carry):
            who = lax.rem(c + 1 + n, G)
            for j in range(r):
                chunk(s, first, who, j)

            @pl.when(s == z)
            def _():
                finish(n, who)

            return carry

        late = G - early
        per = G // late
        for k in range(late):
            lax.fori_loop(k * per, (k + 1) * per if k < late - 1 else G, body, 0)
            pass_on(s + 1, early + k)

    attend(0, True)

    def step(s, carry):
        for g in range(early):
            pass_on(s + 1, g)
        attend(s, False)
        return carry

    lax.fori_loop(1, z + 1, step, 0)

    abuf[c] = obox[G - 1]
    lbuf[c] = lbox[G - 1]
    wo_copy.wait()
    for n in range(G - 1):
        back(0, n).wait_recv()
        back(1, n).wait_recv()
    for a in range(G):
        lse_out[a * r : (a + 1) * r, :] = lbuf[a, 0:r, :]

    piece = R // T

    def share(dest):
        rows = pl.ds(pl.multiple_of(dest * piece, piece), piece)
        total = None
        for a in range(G):
            term = jnp.dot(
                abuf[a, rows, :],
                wo[a * span : (a + 1) * span, :],
                preferred_element_type=jnp.float32,
            )
            total = term if total is None else total + term
        return total.astype(jnp.bfloat16)

    hops = []
    for o in range(1, T):
        dest = lax.rem(t + o, T)
        sbox[o] = share(dest)
        copy = pltpu.make_async_remote_copy(
            src_ref=sbox.at[o],
            dst_ref=rbox.at[o],
            send_sem=tp_send.at[o],
            recv_sem=tp_recv.at[o],
            device_id={"tp": dest},
            device_id_type=MESH,
        )
        copy.start()
        hops.append(copy)
    final = share(t).astype(jnp.float32)
    for o in range(1, T):
        hops[o - 1].wait_recv()
        final = final + rbox[o].astype(jnp.float32)
    mixed[...] = final.astype(jnp.bfloat16)

    for copy in hops:
        copy.wait_send()
    for g in range(1, G):
        for i in range(5):
            swap(i, g).wait_send()
        for i in range(2):
            back(i, g - 1).wait_send()

    @pl.when(z + 1 < Z)
    def _():
        def drain(s, carry):
            for g in range(G):
                for copy in chain(s, g):
                    copy.wait_send()
            return carry

        lax.fori_loop(0, z + 1, drain, 0)


def shards(
    tokens,
    query_weight,
    key_matrix,
    value_matrix,
    gate_weight,
    key_pool_weight,
    value_pool_weight,
    out_weight,
    chosen,
):
    R, width = tokens.shape
    kv_size = lax.axis_size("kv")
    T = lax.axis_size("tp")
    kv = lax.axis_index("kv")
    t = lax.axis_index("tp")
    G = key_matrix.shape[1] // HEAD_SIZE
    r = query_weight.shape[1] // key_matrix.shape[1]
    Z = kv_size // G
    H = gate_weight.shape[2]
    per_dev = chosen.shape[0]
    pooled = R // POOL_STRIDE
    nb = G * per_dev
    nbp = max(8, nb)
    span = r * HEAD_SIZE
    f32, bf16 = jnp.float32, jnp.bfloat16

    half = HEAD_SIZE // 2
    lane = jnp.arange(HEAD_SIZE, dtype=jnp.int32)
    inverse = THETA ** (-(lane % half).astype(f32) / half)
    positions = kv * R + jnp.arange(R, dtype=jnp.int32)
    angles = positions.astype(f32)[:, None] * inverse[None, :]
    cos = jnp.cos(angles)
    sin = jnp.sin(angles) * jnp.where(lane < half, -1.0, 1.0)[None, :]
    blocks = jnp.arange(kv_size * per_dev, dtype=jnp.int32)
    counts = jnp.sum((chosen[None] == blocks[:, None, None]).astype(f32), axis=2)
    counts = jnp.pad(counts.reshape(Z, nb, per_dev), ((0, 0), (0, nbp - nb), (0, 128 - per_dev)))

    vmem = pl.BlockSpec(memory_space=pltpu.VMEM)
    anywhere = pl.BlockSpec(memory_space=pl.ANY)
    sem = pltpu.SemaphoreType.DMA
    keys_shape = (R + 2 * pooled, HEAD_SIZE)
    out_width = out_weight.shape[1]
    mixed, lse = pl.pallas_call(
        functools.partial(attend_kernel, (G, Z, T, R, r, H)),
        in_specs=[anywhere] * 6 + [vmem] * 5,
        out_specs=[vmem, vmem],
        out_shape=[
            jax.ShapeDtypeStruct((R // T, out_width), bf16),
            jax.ShapeDtypeStruct((G * r, R), f32),
        ],
        scratch_shapes=[
            pltpu.VMEM((R, width), bf16),
            pltpu.VMEM((G, width, span), bf16),
            pltpu.VMEM((G, width, 2 * HEAD_SIZE), bf16),
            pltpu.VMEM(out_weight.shape, bf16),
            pltpu.VMEM((G, R, span), bf16),
            pltpu.VMEM((G, *keys_shape), bf16),
            pltpu.VMEM((G, HEAD_SIZE, R), bf16),
            pltpu.VMEM((2 * H, R), f32),
            pltpu.VMEM((G, R, span), bf16),
            pltpu.VMEM((Z, G, *keys_shape), bf16),
            pltpu.VMEM((Z, G, HEAD_SIZE, R), bf16),
            pltpu.VMEM((G, Z, nbp, 128), f32),
            pltpu.VMEM((G, 2 * H, R), f32),
            pltpu.VMEM((G, Z, nbp, R), f32),
            pltpu.VMEM((G, r, HEAD_SIZE, R), f32),
            pltpu.VMEM((G, r, 1, R), f32),
            pltpu.VMEM((G, r, 1, R), f32),
            pltpu.VMEM((G, r, HEAD_SIZE, R), f32),
            pltpu.VMEM((G, r, 1, R), f32),
            pltpu.VMEM((G, r, 1, R), f32),
            pltpu.VMEM((G, R, span), bf16),
            pltpu.VMEM((G, 8, R), f32),
            pltpu.VMEM((G, R, span), bf16),
            pltpu.VMEM((G, 8, R), f32),
            pltpu.VMEM((T, R // T, out_width), bf16),
            pltpu.VMEM((T, R // T, out_width), bf16),
            sem((3,)),
            sem((3, G)),
            sem((5, G)),
            sem((5, G)),
            sem((2, Z, G)),
            sem((2, Z, G)),
            sem((2, G)),
            sem((2, G)),
            sem((T,)),
            sem((T,)),
        ],
        compiler_params=pltpu.CompilerParams(collective_id=0, has_side_effects=True),
        name="attend",
    )(
        tokens,
        query_weight,
        key_matrix,
        value_matrix,
        out_weight,
        counts,
        jnp.swapaxes(gate_weight, 1, 2),
        key_pool_weight.T,
        value_pool_weight.T,
        cos,
        sin,
    )
    return mixed, lse.T


def solution(mesh):
    in_specs = (
        P("kv", None),
        P(None, "tp"),
        P(None, "tp"),
        P(None, "tp"),
        P(),
        P(),
        P(),
        P("tp", None),
        P("kv", None),
    )
    out_specs = (P(("kv", "tp"), None), P("kv", "tp"))
    return jax.shard_map(shards, mesh=mesh, in_specs=in_specs, out_specs=out_specs, check_vma=False)
```
